32 devices in a mesh: grp: 2 (over y), ep: 8 (over z, x), tp: 2 (over core).
Axes of the slice: x: 2, y: 2, z: 4, core: 2. Of those that a mesh axis runs over, the one named last changes fastest.
Arguments:
- tokens: bfloat16 [384, 2048], P(('grp', 'ep')), parts along dimension 0, may hold values from -6 to 6
- norm_gain: float32 [2048], replicated, may hold values from 0.1 to 1.9
- routes: int32 [384, 4], P(('grp', 'ep')), parts along dimension 0, may hold values from 0 to 7, all different within a row; in each aligned block of 24 rows (0 to 23, 24 to 47, ...) at most 24 rows name the same one
- gate_scores: float32 [384, 4], P(('grp', 'ep')), parts along dimension 0, may hold values from 0.05 to 1
- w_gate: bfloat16 [8, 2048, 512], P('ep', None, 'tp'), may hold values from -1 to 1
- w_up: bfloat16 [8, 2048, 512], P('ep', None, 'tp'), may hold values from -1 to 1
- w_down: bfloat16 [8, 512, 2048], P('ep', 'tp'), may hold values from -0.0625 to 0.0625
Outputs:
- mixed: bfloat16 [384, 2048], P(('grp', 'ep')), parts along dimension 0
The draws below stay inside these ranges and needn't reach their ends.
There are 2 independent parts, one for each index of `grp`. The reference program is written for one: setup_inputs(seed, part) draws one part's arguments, and reference() takes and returns one part's arrays. A program takes and returns all parts, laid end to end along the dimension named above; an argument that names none is the same for every part. Nothing has to cross between parts.
Inputs may be any that keep to these rules, and one draw needn't show every extreme that they name: `routes`: each row names 4 different experts; among the 24 rows of one device no expert is named more than 24 times, a bound that some block reaches.
All inputs are finite; a program needn't handle non-finite values.
Results may differ from the reference program's by a relative error of at most 0.0077.
Values may be sent and summed in bfloat16 or wider, within the bound.
No kernel may reach another device: no remote copies, remote signals or barrier semaphores. Data moves between devices by JAX's collectives and lax.ppermute only.
A program may use at most 64 MiB of HBM per device.

```python
import math
import jax
import jax.numpy as jnp
import numpy as np
from jax import lax

D = 2048
FF = 512
TOP_K = 4
TOK_DEV = 24
EXPERTS = 8
TOKENS = 192
CAP = 24
N_EP = 8
N_TP = 2


def levels(key, shape, cuts, smallest, largest):
    def one(axis_at, blocks):
        draws = jax.random.uniform(jax.random.fold_in(jax.random.fold_in(key, 6), axis_at), (blocks,), jnp.float32, smallest / len(cuts), largest / len(cuts))
        return jnp.repeat(jnp.exp(draws), shape[axis_at] // blocks).reshape((-1,) + (1,) * (len(shape) - axis_at - 1))

    loudness = one(*cuts[0])
    for cut in cuts[1:]:
        loudness = loudness * one(*cut)
    return loudness


def routed_block(rng, own, number, rows, number_of, top, reach, slope):
    sequence = jax.random.permutation(rng, number_of)
    crowded, ordinary = load_shares(number_of, rows * top, reach, slope, True), load_shares(number_of, rows * top, reach, slope, False)
    places = jnp.arange(number_of)

    def named(sizes, turn):
        used = int((sizes > 0).sum())
        fixed = max(1, used // 4)
        shifted = fixed + (places - fixed + turn * (used - fixed)) % max(1, number_of - fixed)
        return jnp.zeros((number_of,), jnp.int32).at[sequence[jnp.where(places < fixed, places, shifted)]].set(jnp.asarray(sizes, jnp.int32))

    sizes = jnp.where(number % 4 == 0, named(crowded, number // 4), named(ordinary, number - number // 4 - 1))
    mixed = jax.random.permutation(jax.random.fold_in(own, 3), number_of)
    giver, receiver = mixed[0:number_of // 2 * 2:2], mixed[1:number_of // 2 * 2:2]
    margin = jnp.minimum(sizes[giver] - 1, reach - sizes[receiver]) // 2
    margin = jnp.where((giver == sequence[0]) | (receiver == sequence[0]) | (sizes[receiver] == 0), 0, jnp.maximum(margin, 0))
    shifted = jax.random.randint(jax.random.fold_in(own, 4), (number_of // 2,), 0, 1 << 20) % (margin + 1)
    sizes = sizes.at[giver].add(-shifted).at[receiver].add(shifted)
    items = jnp.searchsorted(jnp.cumsum(sizes), jnp.arange(rows * top), side="right").astype(jnp.int32)
    table = items.reshape(top, rows).T
    table = table[jax.random.permutation(jax.random.fold_in(own, 1), rows)]
    turn = jax.random.randint(jax.random.fold_in(own, 2), (rows, 1), 0, top)
    return jnp.take_along_axis(table, (jnp.arange(top)[None, :] + turn) % top, axis=1)


def load_shares(number_of, total, reach, lean, full):
    weights = [(1 << 20) // math.isqrt(standing ** lean) + 1 for standing in range(1, number_of + 1)]
    largest = reach if full else min(reach, max(-(-total // number_of), total * weights[0] // sum(weights)))
    least = 1 if total - largest >= number_of - 1 else 0
    given, spare = [largest] + [least] * (number_of - 1), total - largest - least * (number_of - 1)
    while spare > 0:
        movable = [i for i in range(1, number_of) if given[i] < largest] or [i for i in range(1, number_of) if given[i] < reach]
        whole, budget = sum([weights[i] for i in movable]), spare
        for i in movable:
            addition = min(reach - given[i], max(1, budget * weights[i] // whole), spare)
            given[i] = given[i] + addition
            spare = spare - addition
    return np.array(given)


def bell_draw(own_key, dims, spread, reach, shards=(), held_as=jnp.bfloat16):
    entries = spread * jax.random.normal(own_key, dims, jnp.float32)
    if shards:
        entries = entries * levels(own_key, dims, shards, -0.22, 0.18)
    return jnp.clip(entries, -reach, reach).astype(held_as)


def setup_inputs(seed: int = 0, part: int = 0) -> dict:
    seeds = jax.random.split(jax.random.key(seed), 8)
    part_keys = jax.random.split(jax.random.fold_in(seeds[7], part), 8)
    tokens = bell_draw(part_keys[0], (TOKENS, D), 1.0, 6.0, ((0, 8),))
    norm_gain = jnp.clip(1.0 + 0.18 * jax.random.normal(seeds[1], (D,), jnp.float32), 0.1, 1.9)
    routes_keys = jax.random.split(jax.random.fold_in(part_keys[2], 1), TOKENS // TOK_DEV)
    routes_turns = jax.random.permutation(jax.random.fold_in(part_keys[2], 3), TOKENS // TOK_DEV)
    routes = jax.vmap(lambda own, number: routed_block(jax.random.fold_in(part_keys[2], 2), own, number, TOK_DEV, EXPERTS, TOP_K, CAP, 2))(routes_keys, routes_turns).reshape((TOKENS, TOP_K))
    gate_scores = jnp.clip(0.05 + 0.95 * jax.random.uniform(part_keys[3], (TOKENS, TOP_K), jnp.float32) ** levels(part_keys[3], (TOKENS, TOP_K), ((0, 8),), -0.2, 0.2), 0.05, 1.0)
    w_gate = bell_draw(seeds[4], (EXPERTS, D, FF), (3 * D ** -0.5), 1.0, ((0, 8), (2, 2)))
    w_up = bell_draw(seeds[5], (EXPERTS, D, FF), (3 * D ** -0.5), 1.0, ((0, 8), (2, 2)))
    w_down = bell_draw(seeds[6], (EXPERTS, FF, D), (16 * FF) ** -0.5, 0.0625, ((0, 8), (1, 2)))
    return {"tokens": tokens, "norm_gain": norm_gain, "routes": routes, "gate_scores": gate_scores, "w_gate": w_gate, "w_up": w_up, "w_down": w_down}


def clamped_unit(g, u):
    gate = jnp.minimum(g, 7.0)
    up = jnp.clip(u, -7.0, 7.0)
    return (up + 1.0) * gate * jax.nn.sigmoid(1.702 * gate)

def expert_apply(rows, wg, wu, wd):
    g = jnp.dot(rows, wg, preferred_element_type=jnp.float32)
    u = jnp.dot(rows, wu, preferred_element_type=jnp.float32)
    act = clamped_unit(g, u).astype(jnp.bfloat16)
    count = rows.shape[0]
    width = wd.shape[0]
    act_groups = act.reshape(count, N_TP, width // N_TP).astype(jnp.float32)
    down_groups = wd.reshape(N_TP, width // N_TP, wd.shape[1]).astype(jnp.float32)
    parts = jnp.einsum('rnf,nfd->nrd', act_groups, down_groups)
    parts = lax.optimization_barrier(parts.astype(jnp.bfloat16)).astype(jnp.float32)
    return lax.optimization_barrier(jnp.sum(parts, axis=0)).astype(jnp.bfloat16)

def reference(tokens, norm_gain, routes, gate_scores, w_gate, w_up, w_down):
    xf = tokens.astype(jnp.float32)
    normed = (xf * lax.rsqrt(lax.optimization_barrier(jnp.mean(xf * xf, axis=-1, keepdims=True)) + 1e-06) * norm_gain).astype(jnp.bfloat16)
    count = tokens.shape[0]
    width = tokens.shape[1]
    padded = jnp.concatenate([normed, jnp.zeros((1, width), jnp.bfloat16)], axis=0)
    slots = N_EP * CAP

    def one_expert(total, inputs):
        wg, wu, wd, expert = inputs
        chosen = routes == expert
        hit = jnp.any(chosen, axis=1)
        weight = lax.optimization_barrier(jnp.sum(jnp.where(chosen, gate_scores, 0.0), axis=1))
        weight = jnp.concatenate([weight, jnp.zeros((1,), jnp.float32)])
        index = jnp.nonzero(hit, size=slots, fill_value=count)[0].astype(jnp.int32)
        outputs = expert_apply(padded[index], wg, wu, wd)
        contrib = weight[index][:, None] * outputs.astype(jnp.float32)
        return (total.at[index].add(contrib), None)
    start = jnp.zeros((count + 1, width), jnp.float32)
    experts = jnp.arange(w_gate.shape[0], dtype=jnp.int32)
    total, _ = lax.scan(one_expert, start, (w_gate, w_up, w_down, experts))
    return total[:count].astype(jnp.bfloat16)
```

```python
import jax
import jax.numpy as jnp
from jax import lax
from jax.sharding import PartitionSpec as P


def clamped_unit(g, u):
    gate = jnp.minimum(g, 7.0)
    up = jnp.clip(u, -7.0, 7.0)
    return (up + 1.0) * gate * jax.nn.sigmoid(1.702 * gate)


def expert_rows(rows, wg, wu, wd):
    g = jnp.dot(rows, wg, preferred_element_type=jnp.float32)
    u = jnp.dot(rows, wu, preferred_element_type=jnp.float32)
    act = clamped_unit(g, u).astype(jnp.bfloat16)
    part = jnp.dot(act, wd, preferred_element_type=jnp.float32)
    part = lax.optimization_barrier(part.astype(jnp.bfloat16)).astype(jnp.float32)
    total = lax.psum(part.astype(jnp.bfloat16), "tp")
    return total


def finish(mixed):
    result = mixed.astype(jnp.bfloat16)
    return result


def normalise(tokens, norm_gain):
    xf = tokens.astype(jnp.float32)
    scale = lax.rsqrt(jnp.mean(xf * xf, axis=-1, keepdims=True) + 1e-06)
    return (xf * scale * norm_gain).astype(jnp.bfloat16)


def slot_table(routes, scores, experts, capacity):
    count = routes.shape[0]
    chosen = routes[:, :, None] == experts[None, None, :]
    hit = jnp.any(chosen, axis=1).astype(jnp.int32)
    weight = jnp.sum(jnp.where(chosen, scores[:, :, None], 0.0), axis=1)
    rank = jnp.cumsum(hit, axis=0) - hit
    places = jnp.arange(capacity, dtype=jnp.int32)
    match = (hit[:, :, None] == 1) & (rank[:, :, None] == places[None, None, :])
    row_ids = jnp.arange(count, dtype=jnp.int32)[:, None, None]
    filled = jnp.any(match, axis=0)
    slot_tok = jnp.sum(jnp.where(match, row_ids, 0), axis=0) + count * (
        1 - filled.astype(jnp.int32)
    )
    slot_w = jnp.sum(jnp.where(match, weight[:, :, None], 0.0), axis=0)
    return (slot_tok, slot_w)


def slotted(tokens, norm_gain, routes, gate_scores, w_gate, w_up, w_down, capacity):
    count, width = tokens.shape
    nexp = lax.axis_size("ep")
    wg, wu, wd = (w_gate[0], w_up[0], w_down[0])
    normed = normalise(tokens, norm_gain)
    experts = jnp.arange(nexp, dtype=jnp.int32)
    slot_tok, slot_w = slot_table(routes, gate_scores, experts, capacity)
    padded = jnp.concatenate([normed, jnp.zeros((1, width), jnp.bfloat16)], axis=0)
    outgoing = padded[slot_tok]
    received = lax.all_to_all(outgoing, "ep", split_axis=0, concat_axis=0, tiled=True)
    sources, places, _ = received.shape
    outputs = expert_rows(received.reshape(sources * places, width), wg, wu, wd)
    returned = lax.all_to_all(
        outputs.reshape(sources, places, outputs.shape[1]),
        "ep",
        split_axis=0,
        concat_axis=0,
        tiled=True,
    )
    flat_tok = slot_tok.reshape(-1)
    token_ids = jnp.arange(count, dtype=jnp.int32)
    combine = jnp.where(flat_tok[None, :] == token_ids[:, None], slot_w.reshape(-1)[None, :], 0.0)
    mixed = jnp.dot(
        combine,
        returned.reshape(-1, returned.shape[2]).astype(jnp.float32),
        precision=lax.Precision.HIGHEST,
    )
    return finish(mixed)


def swap(x, axis, mask):
    size = lax.axis_size(axis)
    return lax.ppermute(x, axis, [(i, i ^ mask) for i in range(size)])


def dense(tokens, norm_gain, routes, gate_scores, w_gate, w_up, w_down):
    count, width = tokens.shape
    nexp = lax.axis_size("ep")
    half = width // 2
    tp = lax.axis_index("tp")
    wg, wu, wd = (w_gate[0], w_up[0], w_down[0])
    masks = [1 << b for b in reversed(range((nexp - 1).bit_length()))]

    lanes = -(-nexp // 128) * 128
    experts = jnp.arange(lanes, dtype=jnp.int32)
    chosen = routes[:, :, None] == experts[None, None, :]
    weight = jnp.sum(jnp.where(chosen, gate_scores[:, :, None], 0.0), axis=1)
    high = weight.astype(jnp.bfloat16)
    low = (weight - lax.reduce_precision(weight, 8, 7)).astype(jnp.bfloat16)

    xf = tokens.astype(jnp.float32)
    scale = lax.rsqrt(jnp.mean(xf * xf, axis=-1, keepdims=True) + 1e-06)
    own_x = lax.dynamic_slice_in_dim(xf, tp * half, half, 1)
    own_gain = lax.dynamic_slice_in_dim(norm_gain, tp * half, half, 0)
    normed = (own_x * scale * own_gain).astype(jnp.bfloat16)
    rows = jnp.concatenate([normed, jnp.where(tp == 0, high, low)], axis=1)
    for mask in masks:
        rows = jnp.concatenate([rows, swap(rows, "ep", mask)], axis=0)
    both = lax.all_gather(rows, "tp")
    full = jnp.concatenate([both[0, :, :half], both[1, :, :half]], axis=1)
    pair = both[0, :, half:].astype(jnp.float32) + both[1, :, half:].astype(jnp.float32)
    mine = (experts == lax.axis_index("ep"))[None, :]
    score = jnp.sum(jnp.where(mine, pair, 0.0), axis=1, keepdims=True)

    g = jnp.dot(full, wg, preferred_element_type=jnp.float32)
    u = jnp.dot(full, wu, preferred_element_type=jnp.float32)
    act = clamped_unit(g, u).astype(jnp.bfloat16)
    wd_own = lax.dynamic_slice_in_dim(wd, tp * half, half, 1)
    wd_other = lax.dynamic_slice_in_dim(wd, (1 - tp) * half, half, 1)
    other = jnp.dot(act, wd_other, preferred_element_type=jnp.float32).astype(jnp.bfloat16)
    other = swap(other, "tp", 1)
    own = jnp.dot(act, wd_own, preferred_element_type=jnp.float32)
    total = (own + other.astype(jnp.float32)) * score
    for mask in reversed(masks):
        n = total.shape[0] // 2
        sent = swap(total[n:].astype(jnp.bfloat16), "ep", mask)
        total = total[:n] + sent.astype(jnp.float32)
    mixed = finish(total)
    theirs = swap(mixed, "tp", 1)
    return jnp.concatenate(
        [jnp.where(tp == 0, mixed, theirs), jnp.where(tp == 0, theirs, mixed)], axis=1
    )


def body(tokens, norm_gain, routes, gate_scores, w_gate, w_up, w_down):
    args = (tokens, norm_gain, routes, gate_scores, w_gate, w_up, w_down)
    count = tokens.shape[0]
    top = routes.shape[1]
    nexp = lax.axis_size("ep")
    capacity = max(2, min(count, 2 * count * top // nexp))
    if capacity == count and nexp & (nexp - 1) == 0 and lax.axis_size("tp") == 2:
        return dense(*args)
    return slotted(*args, capacity)


def solution(mesh):
    in_specs = (
        P(("grp", "ep"), None),
        P(),
        P(("grp", "ep"), None),
        P(("grp", "ep"), None),
        P("ep", None, "tp"),
        P("ep", None, "tp"),
        P("ep", "tp", None),
    )
    out_specs = P(("grp", "ep"), None)
    return jax.shard_map(body, mesh=mesh, in_specs=in_specs, out_specs=out_specs, check_vma=False)
```

```python
import jax
import jax.numpy as jnp
from jax import lax
from jax.experimental import pallas as pl
from jax.sharding import PartitionSpec as P


def clamped_unit(g, u):
    gate = jnp.minimum(g, 7.0)
    up = jnp.clip(u, -7.0, 7.0)
    return (up + 1.0) * gate * jax.nn.sigmoid(1.702 * gate)


def expert_rows(rows, wg, wu, wd):
    g = jnp.dot(rows, wg, preferred_element_type=jnp.float32)
    u = jnp.dot(rows, wu, preferred_element_type=jnp.float32)
    act = clamped_unit(g, u).astype(jnp.bfloat16)
    part = jnp.dot(act, wd, preferred_element_type=jnp.float32)
    part = lax.optimization_barrier(part.astype(jnp.bfloat16)).astype(jnp.float32)
    total = lax.psum(part.astype(jnp.bfloat16), "tp")
    return total


def finish(mixed):
    result = mixed.astype(jnp.bfloat16)
    return result


def normalise(tokens, norm_gain):
    xf = tokens.astype(jnp.float32)
    scale = lax.rsqrt(jnp.mean(xf * xf, axis=-1, keepdims=True) + 1e-06)
    return (xf * scale * norm_gain).astype(jnp.bfloat16)


def slot_table(routes, scores, experts, capacity):
    count = routes.shape[0]
    chosen = routes[:, :, None] == experts[None, None, :]
    hit = jnp.any(chosen, axis=1).astype(jnp.int32)
    weight = jnp.sum(jnp.where(chosen, scores[:, :, None], 0.0), axis=1)
    rank = jnp.cumsum(hit, axis=0) - hit
    places = jnp.arange(capacity, dtype=jnp.int32)
    match = (hit[:, :, None] == 1) & (rank[:, :, None] == places[None, None, :])
    row_ids = jnp.arange(count, dtype=jnp.int32)[:, None, None]
    filled = jnp.any(match, axis=0)
    slot_tok = jnp.sum(jnp.where(match, row_ids, 0), axis=0) + count * (
        1 - filled.astype(jnp.int32)
    )
    slot_w = jnp.sum(jnp.where(match, weight[:, :, None], 0.0), axis=0)
    return (slot_tok, slot_w)


def slotted(tokens, norm_gain, routes, gate_scores, w_gate, w_up, w_down, capacity):
    count, width = tokens.shape
    nexp = lax.axis_size("ep")
    wg, wu, wd = (w_gate[0], w_up[0], w_down[0])
    normed = normalise(tokens, norm_gain)
    experts = jnp.arange(nexp, dtype=jnp.int32)
    slot_tok, slot_w = slot_table(routes, gate_scores, experts, capacity)
    padded = jnp.concatenate([normed, jnp.zeros((1, width), jnp.bfloat16)], axis=0)
    outgoing = padded[slot_tok]
    received = lax.all_to_all(outgoing, "ep", split_axis=0, concat_axis=0, tiled=True)
    sources, places, _ = received.shape
    outputs = expert_rows(received.reshape(sources * places, width), wg, wu, wd)
    returned = lax.all_to_all(
        outputs.reshape(sources, places, outputs.shape[1]),
        "ep",
        split_axis=0,
        concat_axis=0,
        tiled=True,
    )
    flat_tok = slot_tok.reshape(-1)
    token_ids = jnp.arange(count, dtype=jnp.int32)
    combine = jnp.where(flat_tok[None, :] == token_ids[:, None], slot_w.reshape(-1)[None, :], 0.0)
    mixed = jnp.dot(
        combine,
        returned.reshape(-1, returned.shape[2]).astype(jnp.float32),
        precision=lax.Precision.HIGHEST,
    )
    return finish(mixed)


def swap(x, mask):
    nexp, cores = lax.axis_size("ep"), lax.axis_size("tp")
    if mask is None:
        return lax.ppermute(x, "tp", [(c, c ^ 1) for c in range(cores)])
    pairs = [(e * cores + c, (e ^ mask[c]) * cores + c) for e in range(nexp) for c in range(cores)]
    return lax.ppermute(x, ("ep", "tp"), pairs)


def prepare(tokens, norm_gain, routes, gate_scores, lanes):
    count, width = tokens.shape
    half = width // 2
    top = routes.shape[1]

    def kernel(x_ref, gain_ref, route_ref, score_ref, out_ref):
        first = lax.axis_index("tp") == 0
        x = x_ref[...].astype(jnp.float32)
        scale = lax.rsqrt(jnp.mean(x * x, axis=-1, keepdims=True) + 1e-06)
        normed = x * scale * gain_ref[...]
        out_ref[:, :half] = jnp.where(first, normed[:, :half], normed[:, half:]).astype(jnp.bfloat16)
        expert = lax.broadcasted_iota(jnp.int32, (lanes, count), 0)
        weight = jnp.zeros((lanes, count), jnp.float32)
        for k in range(top):
            weight += jnp.where(route_ref[k : k + 1, :] == expert, score_ref[k : k + 1, :], 0.0)
        high = weight.astype(jnp.bfloat16)
        low = (weight - high.astype(jnp.float32)).astype(jnp.bfloat16)
        term = jnp.where(first, high.astype(jnp.float32), low.astype(jnp.float32)).astype(jnp.bfloat16)
        row = lax.broadcasted_iota(jnp.int32, (lanes, lanes), 0)
        col = lax.broadcasted_iota(jnp.int32, (lanes, lanes), 1)
        unit = jnp.where(row == col, 1.0, 0.0).astype(jnp.bfloat16)
        turned = lax.dot_general(term, unit, (((0,), (0,)), ((), ())), preferred_element_type=jnp.float32)
        out_ref[:, half:] = turned.astype(jnp.bfloat16)

    return pl.pallas_call(
        kernel,
        out_shape=jax.ShapeDtypeStruct((count, half + lanes), jnp.bfloat16),
        name="prepare",
    )(tokens, norm_gain[None, :], routes.T, gate_scores.T)


def dense(tokens, norm_gain, routes, gate_scores, w_gate, w_up, w_down):
    width = tokens.shape[1]
    nexp = lax.axis_size("ep")
    half = width // 2
    hidden = w_gate.shape[2]
    tp = lax.axis_index("tp")
    first = tp == 0
    masks = [1 << b for b in reversed(range((nexp - 1).bit_length()))]
    steps = list(zip(masks, masks[:-2] + masks[-1:] + masks[-2:-1]))
    lanes = -(-nexp // 128) * 128

    rows = prepare(tokens, norm_gain, routes, gate_scores, lanes)

    def own_first(w, axis):
        own = lax.dynamic_slice_in_dim(w, tp * half, half, axis)
        return own, lax.dynamic_slice_in_dim(w, (1 - tp) * half, half, axis)

    gate_own, gate_other = own_first(w_gate[0], 0)
    up_own, up_other = own_first(w_up[0], 0)
    in_own = jnp.concatenate([gate_own, up_own], axis=1)
    in_other = jnp.concatenate([gate_other, up_other], axis=1)
    down_own, down_other = own_first(w_down[0], 1)

    for mask in steps[:-1]:
        rows = jnp.concatenate([rows, swap(rows, mask)], axis=0)
    far = swap(rows, steps[-1])
    in_own, in_other, down_own, down_other = lax.optimization_barrier(
        (in_own, in_other, down_own, down_other)
    )
    n = rows.shape[0] // 2
    one, two = rows[n:], far[:n]
    own = jnp.concatenate(
        [rows[:n], jnp.where(first, one, two), jnp.where(first, two, one), far[n:]], axis=0
    )
    other = swap(own, None)
    h = jnp.dot(own[:, :half], in_own, preferred_element_type=jnp.float32)
    h = h + jnp.dot(other[:, :half], in_other, preferred_element_type=jnp.float32)
    pair = own[:, half:].astype(jnp.float32) + other[:, half:].astype(jnp.float32)
    mine = (jnp.arange(lanes, dtype=jnp.int32) == lax.axis_index("ep"))[None, :]
    score = jnp.sum(jnp.where(mine, pair, 0.0), axis=1, keepdims=True)
    act = clamped_unit(h[:, :hidden], h[:, hidden:]).astype(jnp.bfloat16)

    given = jnp.dot(act, down_other, preferred_element_type=jnp.float32).astype(jnp.bfloat16)
    taken = swap(given, None)
    kept = jnp.dot(act, down_own, preferred_element_type=jnp.float32)
    total = (kept + taken.astype(jnp.float32)) * score
    one, two = total[n : 2 * n], total[2 * n : 3 * n]
    near = jnp.concatenate([total[:n], jnp.where(first, one, two)], axis=0)
    far = jnp.concatenate([jnp.where(first, two, one), total[3 * n :]], axis=0)
    for mask in reversed(steps):
        near = near + swap(far.astype(jnp.bfloat16), mask).astype(jnp.float32)
        n = near.shape[0] // 2
        if mask is not steps[0]:
            near, far = near[:n], near[n:]
    mixed = finish(near)
    theirs = swap(mixed, None)
    return jnp.concatenate(
        [jnp.where(first, mixed, theirs), jnp.where(first, theirs, mixed)], axis=1
    )


def body(tokens, norm_gain, routes, gate_scores, w_gate, w_up, w_down):
    args = (tokens, norm_gain, routes, gate_scores, w_gate, w_up, w_down)
    count = tokens.shape[0]
    top = routes.shape[1]
    nexp = lax.axis_size("ep")
    capacity = max(2, min(count, 2 * count * top // nexp))
    if capacity == count and nexp >= 4 and nexp & (nexp - 1) == 0 and lax.axis_size("tp") == 2:
        return dense(*args)
    return slotted(*args, capacity)


def solution(mesh):
    in_specs = (
        P(("grp", "ep"), None),
        P(),
        P(("grp", "ep"), None),
        P(("grp", "ep"), None),
        P("ep", None, "tp"),
        P("ep", None, "tp"),
        P("ep", "tp", None),
    )
    out_specs = P(("grp", "ep"), None)
    return jax.shard_map(body, mesh=mesh, in_specs=in_specs, out_specs=out_specs, check_vma=False)
```

```python
import jax
import jax.numpy as jnp
from jax import lax
from jax.experimental import pallas as pl
from jax.experimental.pallas import tpu as pltpu
from jax.sharding import PartitionSpec as P


def clamped_unit(g, u):
    gate = jnp.minimum(g, 7.0)
    up = jnp.clip(u, -7.0, 7.0)
    return (up + 1.0) * gate * jax.nn.sigmoid(1.702 * gate)


def expert_rows(rows, wg, wu, wd):
    g = jnp.dot(rows, wg, preferred_element_type=jnp.float32)
    u = jnp.dot(rows, wu, preferred_element_type=jnp.float32)
    act = clamped_unit(g, u).astype(jnp.bfloat16)
    part = jnp.dot(act, wd, preferred_element_type=jnp.float32)
    part = lax.optimization_barrier(part.astype(jnp.bfloat16)).astype(jnp.float32)
    total = lax.psum(part.astype(jnp.bfloat16), "tp")
    return total


def finish(mixed):
    result = mixed.astype(jnp.bfloat16)
    return result


def normalise(tokens, norm_gain):
    xf = tokens.astype(jnp.float32)
    scale = lax.rsqrt(jnp.mean(xf * xf, axis=-1, keepdims=True) + 1e-06)
    return (xf * scale * norm_gain).astype(jnp.bfloat16)


def slot_table(routes, scores, experts, capacity):
    count = routes.shape[0]
    chosen = routes[:, :, None] == experts[None, None, :]
    hit = jnp.any(chosen, axis=1).astype(jnp.int32)
    weight = jnp.sum(jnp.where(chosen, scores[:, :, None], 0.0), axis=1)
    rank = jnp.cumsum(hit, axis=0) - hit
    places = jnp.arange(capacity, dtype=jnp.int32)
    match = (hit[:, :, None] == 1) & (rank[:, :, None] == places[None, None, :])
    row_ids = jnp.arange(count, dtype=jnp.int32)[:, None, None]
    filled = jnp.any(match, axis=0)
    slot_tok = jnp.sum(jnp.where(match, row_ids, 0), axis=0) + count * (
        1 - filled.astype(jnp.int32)
    )
    slot_w = jnp.sum(jnp.where(match, weight[:, :, None], 0.0), axis=0)
    return (slot_tok, slot_w)


def slotted(tokens, norm_gain, routes, gate_scores, w_gate, w_up, w_down, capacity):
    count, width = tokens.shape
    nexp = lax.axis_size("ep")
    wg, wu, wd = (w_gate[0], w_up[0], w_down[0])
    normed = normalise(tokens, norm_gain)
    experts = jnp.arange(nexp, dtype=jnp.int32)
    slot_tok, slot_w = slot_table(routes, gate_scores, experts, capacity)
    padded = jnp.concatenate([normed, jnp.zeros((1, width), jnp.bfloat16)], axis=0)
    outgoing = padded[slot_tok]
    received = lax.all_to_all(outgoing, "ep", split_axis=0, concat_axis=0, tiled=True)
    sources, places, _ = received.shape
    outputs = expert_rows(received.reshape(sources * places, width), wg, wu, wd)
    returned = lax.all_to_all(
        outputs.reshape(sources, places, outputs.shape[1]),
        "ep",
        split_axis=0,
        concat_axis=0,
        tiled=True,
    )
    flat_tok = slot_tok.reshape(-1)
    token_ids = jnp.arange(count, dtype=jnp.int32)
    combine = jnp.where(flat_tok[None, :] == token_ids[:, None], slot_w.reshape(-1)[None, :], 0.0)
    mixed = jnp.dot(
        combine,
        returned.reshape(-1, returned.shape[2]).astype(jnp.float32),
        precision=lax.Precision.HIGHEST,
    )
    return finish(mixed)


def swap(x, mask):
    nexp, cores = lax.axis_size("ep"), lax.axis_size("tp")
    if mask is None:
        return lax.ppermute(x, "tp", [(c, c ^ 1) for c in range(cores)])
    pairs = [(e * cores + c, (e ^ mask[c]) * cores + c) for e in range(nexp) for c in range(cores)]
    return lax.ppermute(x, ("ep", "tp"), pairs)


def prepare(tokens, norm_gain, routes, gate_scores, lanes):
    count, width = tokens.shape
    half = width // 2
    top = routes.shape[1]

    def kernel(x_ref, gain_ref, route_ref, score_ref, out_ref):
        first = lax.axis_index("tp") == 0
        x = x_ref[...].astype(jnp.float32)
        scale = lax.rsqrt(jnp.mean(x * x, axis=-1, keepdims=True) + 1e-06)
        normed = x * scale * gain_ref[...]
        out_ref[:, :half] = jnp.where(first, normed[:, :half], normed[:, half:]).astype(jnp.bfloat16)
        expert = lax.broadcasted_iota(jnp.int32, (lanes, count), 0)
        weight = jnp.zeros((lanes, count), jnp.float32)
        for k in range(top):
            weight += jnp.where(route_ref[k : k + 1, :] == expert, score_ref[k : k + 1, :], 0.0)
        high = weight.astype(jnp.bfloat16)
        low = (weight - high.astype(jnp.float32)).astype(jnp.bfloat16)
        term = jnp.where(first, high.astype(jnp.float32), low.astype(jnp.float32)).astype(jnp.bfloat16)
        row = lax.broadcasted_iota(jnp.int32, (lanes, lanes), 0)
        col = lax.broadcasted_iota(jnp.int32, (lanes, lanes), 1)
        unit = jnp.where(row == col, 1.0, 0.0).astype(jnp.bfloat16)
        turned = lax.dot_general(term, unit, (((0,), (0,)), ((), ())), preferred_element_type=jnp.float32)
        out_ref[:, half:] = turned.astype(jnp.bfloat16)

    return pl.pallas_call(
        kernel,
        out_shape=pltpu.VMEM((count, half + lanes), jnp.bfloat16),
        compiler_params=pltpu.CompilerParams(vmem_limit_bytes=4 << 20),
        name="prepare",
    )(tokens, norm_gain[None, :], routes.T, gate_scores.T)


def dense(tokens, norm_gain, routes, gate_scores, w_gate, w_up, w_down):
    width = tokens.shape[1]
    nexp = lax.axis_size("ep")
    half = width // 2
    hidden = w_gate.shape[2]
    tp = lax.axis_index("tp")
    first = tp == 0
    masks = [1 << b for b in reversed(range((nexp - 1).bit_length()))]
    steps = list(zip(masks, masks[:-2] + masks[-1:] + masks[-2:-1]))
    lanes = -(-nexp // 128) * 128

    rows = prepare(tokens, norm_gain, routes, gate_scores, lanes)

    def own_first(w, axis):
        own = lax.dynamic_slice_in_dim(w, tp * half, half, axis)
        return own, lax.dynamic_slice_in_dim(w, (1 - tp) * half, half, axis)

    gate_own, gate_other = own_first(w_gate[0], 0)
    up_own, up_other = own_first(w_up[0], 0)
    in_own = jnp.concatenate([gate_own, up_own], axis=1)
    in_other = jnp.concatenate([gate_other, up_other], axis=1)
    down_own, down_other = own_first(w_down[0], 1)

    for mask in steps[:-1]:
        rows = jnp.concatenate([rows, swap(rows, mask)], axis=0)
    far = swap(rows, steps[-1])
    in_own, in_other, down_own, down_other = lax.optimization_barrier(
        (in_own, in_other, down_own, down_other)
    )
    n = rows.shape[0] // 2
    one, two = rows[n:], far[:n]
    own = jnp.concatenate(
        [rows[:n], jnp.where(first, one, two), jnp.where(first, two, one), far[n:]], axis=0
    )
    other = swap(own, None)
    h = jnp.dot(own[:, :half], in_own, preferred_element_type=jnp.float32)
    h = h + jnp.dot(other[:, :half], in_other, preferred_element_type=jnp.float32)
    pair = own[:, half:].astype(jnp.float32) + other[:, half:].astype(jnp.float32)
    mine = (jnp.arange(lanes, dtype=jnp.int32) == lax.axis_index("ep"))[None, :]
    score = jnp.sum(jnp.where(mine, pair, 0.0), axis=1, keepdims=True)
    act = clamped_unit(h[:, :hidden], h[:, hidden:]).astype(jnp.bfloat16)

    given = jnp.dot(act, down_other, preferred_element_type=jnp.float32).astype(jnp.bfloat16)
    taken = swap(given, None)
    kept = jnp.dot(act, down_own, preferred_element_type=jnp.float32)
    total = (kept + taken.astype(jnp.float32)) * score
    one, two = total[n : 2 * n], total[2 * n : 3 * n]
    near = jnp.concatenate([total[:n], jnp.where(first, one, two)], axis=0)
    far = jnp.concatenate([jnp.where(first, two, one), total[3 * n :]], axis=0)
    for mask in reversed(steps):
        near = near + swap(far.astype(jnp.bfloat16), mask).astype(jnp.float32)
        n = near.shape[0] // 2
        if mask is not steps[0]:
            near, far = near[:n], near[n:]
    mixed = finish(near)
    theirs = swap(mixed, None)
    return jnp.concatenate(
        [jnp.where(first, mixed, theirs), jnp.where(first, theirs, mixed)], axis=1
    )


def body(tokens, norm_gain, routes, gate_scores, w_gate, w_up, w_down):
    args = (tokens, norm_gain, routes, gate_scores, w_gate, w_up, w_down)
    count = tokens.shape[0]
    top = routes.shape[1]
    nexp = lax.axis_size("ep")
    capacity = max(2, min(count, 2 * count * top // nexp))
    if capacity == count and nexp >= 4 and nexp & (nexp - 1) == 0 and lax.axis_size("tp") == 2:
        return dense(*args)
    return slotted(*args, capacity)


def solution(mesh):
    in_specs = (
        P(("grp", "ep"), None),
        P(),
        P(("grp", "ep"), None),
        P(("grp", "ep"), None),
        P("ep", None, "tp"),
        P("ep", None, "tp"),
        P("ep", "tp", None),
    )
    out_specs = P(("grp", "ep"), None)
    return jax.shard_map(body, mesh=mesh, in_specs=in_specs, out_specs=out_specs, check_vma=False)
```

```python
import jax
import jax.numpy as jnp
from jax import lax
from jax.experimental import pallas as pl
from jax.experimental.pallas import tpu as pltpu
from jax.sharding import PartitionSpec as P


def clamped_unit(g, u):
    gate = jnp.minimum(g, 7.0)
    up = jnp.clip(u, -7.0, 7.0)
    return (up + 1.0) * gate * jax.nn.sigmoid(1.702 * gate)


def expert_rows(rows, wg, wu, wd):
    g = jnp.dot(rows, wg, preferred_element_type=jnp.float32)
    u = jnp.dot(rows, wu, preferred_element_type=jnp.float32)
    act = clamped_unit(g, u).astype(jnp.bfloat16)
    part = jnp.dot(act, wd, preferred_element_type=jnp.float32)
    part = lax.optimization_barrier(part.astype(jnp.bfloat16)).astype(jnp.float32)
    total = lax.psum(part.astype(jnp.bfloat16), "tp")
    return total


def finish(mixed):
    result = mixed.astype(jnp.bfloat16)
    return result


def normalise(tokens, norm_gain):
    xf = tokens.astype(jnp.float32)
    scale = lax.rsqrt(jnp.mean(xf * xf, axis=-1, keepdims=True) + 1e-06)
    return (xf * scale * norm_gain).astype(jnp.bfloat16)


def slot_table(routes, scores, experts, capacity):
    count = routes.shape[0]
    chosen = routes[:, :, None] == experts[None, None, :]
    hit = jnp.any(chosen, axis=1).astype(jnp.int32)
    weight = jnp.sum(jnp.where(chosen, scores[:, :, None], 0.0), axis=1)
    rank = jnp.cumsum(hit, axis=0) - hit
    places = jnp.arange(capacity, dtype=jnp.int32)
    match = (hit[:, :, None] == 1) & (rank[:, :, None] == places[None, None, :])
    row_ids = jnp.arange(count, dtype=jnp.int32)[:, None, None]
    filled = jnp.any(match, axis=0)
    slot_tok = jnp.sum(jnp.where(match, row_ids, 0), axis=0) + count * (
        1 - filled.astype(jnp.int32)
    )
    slot_w = jnp.sum(jnp.where(match, weight[:, :, None], 0.0), axis=0)
    return (slot_tok, slot_w)


def slotted(tokens, norm_gain, routes, gate_scores, w_gate, w_up, w_down, capacity):
    count, width = tokens.shape
    nexp = lax.axis_size("ep")
    wg, wu, wd = (w_gate[0], w_up[0], w_down[0])
    normed = normalise(tokens, norm_gain)
    experts = jnp.arange(nexp, dtype=jnp.int32)
    slot_tok, slot_w = slot_table(routes, gate_scores, experts, capacity)
    padded = jnp.concatenate([normed, jnp.zeros((1, width), jnp.bfloat16)], axis=0)
    outgoing = padded[slot_tok]
    received = lax.all_to_all(outgoing, "ep", split_axis=0, concat_axis=0, tiled=True)
    sources, places, _ = received.shape
    outputs = expert_rows(received.reshape(sources * places, width), wg, wu, wd)
    returned = lax.all_to_all(
        outputs.reshape(sources, places, outputs.shape[1]),
        "ep",
        split_axis=0,
        concat_axis=0,
        tiled=True,
    )
    flat_tok = slot_tok.reshape(-1)
    token_ids = jnp.arange(count, dtype=jnp.int32)
    combine = jnp.where(flat_tok[None, :] == token_ids[:, None], slot_w.reshape(-1)[None, :], 0.0)
    mixed = jnp.dot(
        combine,
        returned.reshape(-1, returned.shape[2]).astype(jnp.float32),
        precision=lax.Precision.HIGHEST,
    )
    return finish(mixed)


def swap(x, mask):
    nexp, cores = lax.axis_size("ep"), lax.axis_size("tp")
    if mask is None:
        return lax.ppermute(x, "tp", [(c, c ^ 1) for c in range(cores)])
    pairs = [(e * cores + c, (e ^ mask[c]) * cores + c) for e in range(nexp) for c in range(cores)]
    return lax.ppermute(x, ("ep", "tp"), pairs)


def prepare(tokens, norm_gain, routes, gate_scores, lanes):
    count, width = tokens.shape
    half = width // 2
    top = routes.shape[1]

    def kernel(*refs):
        given, out_ref, local, sem = refs[:4], refs[4], refs[5:9], refs[9]
        copies = [pltpu.make_async_copy(a, b, sem.at[i]) for i, (a, b) in enumerate(zip(given, local))]
        for copy in copies:
            copy.start()
        for copy in copies:
            copy.wait()
        x_ref, gain_ref, route_ref, score_ref = local
        first = lax.axis_index("tp") == 0
        x = x_ref[...].astype(jnp.float32)
        scale = lax.rsqrt(jnp.mean(x * x, axis=-1, keepdims=True) + 1e-06)
        normed = x * scale * gain_ref[...]
        out_ref[:, :half] = jnp.where(first, normed[:, :half], normed[:, half:]).astype(jnp.bfloat16)
        expert = lax.broadcasted_iota(jnp.int32, (lanes, count), 0)
        weight = jnp.zeros((lanes, count), jnp.float32)
        for k in range(top):
            weight += jnp.where(route_ref[k : k + 1, :] == expert, score_ref[k : k + 1, :], 0.0)
        high = weight.astype(jnp.bfloat16)
        low = (weight - high.astype(jnp.float32)).astype(jnp.bfloat16)
        term = jnp.where(first, high.astype(jnp.float32), low.astype(jnp.float32)).astype(jnp.bfloat16)
        row = lax.broadcasted_iota(jnp.int32, (lanes, lanes), 0)
        col = lax.broadcasted_iota(jnp.int32, (lanes, lanes), 1)
        unit = jnp.where(row == col, 1.0, 0.0).astype(jnp.bfloat16)
        turned = lax.dot_general(term, unit, (((0,), (0,)), ((), ())), preferred_element_type=jnp.float32)
        out_ref[:, half:] = turned.astype(jnp.bfloat16)

    args = (tokens, norm_gain[None, :], routes.T, gate_scores.T)
    return pl.pallas_call(
        kernel,
        in_specs=[pl.BlockSpec(memory_space=pltpu.HBM)] * len(args),
        out_shape=pltpu.VMEM((count, half + lanes), jnp.bfloat16),
        scratch_shapes=[pltpu.VMEM(a.shape, a.dtype) for a in args]
        + [pltpu.SemaphoreType.DMA((len(args),))],
        compiler_params=pltpu.CompilerParams(vmem_limit_bytes=4 << 20),
        name="prepare",
    )(*[pltpu.with_memory_space_constraint(a, pltpu.HBM) for a in args])


def dense(tokens, norm_gain, routes, gate_scores, w_gate, w_up, w_down):
    width = tokens.shape[1]
    nexp = lax.axis_size("ep")
    half = width // 2
    hidden = w_gate.shape[2]
    tp = lax.axis_index("tp")
    first = tp == 0
    masks = [1 << b for b in reversed(range((nexp - 1).bit_length()))]
    steps = list(zip(masks, masks[:-2] + masks[-1:] + masks[-2:-1]))
    lanes = -(-nexp // 128) * 128

    rows = prepare(tokens, norm_gain, routes, gate_scores, lanes)

    def own_first(w, axis):
        own = lax.dynamic_slice_in_dim(w, tp * half, half, axis)
        return own, lax.dynamic_slice_in_dim(w, (1 - tp) * half, half, axis)

    gate_own, gate_other = own_first(w_gate[0], 0)
    up_own, up_other = own_first(w_up[0], 0)
    in_own = jnp.concatenate([gate_own, up_own], axis=1)
    in_other = jnp.concatenate([gate_other, up_other], axis=1)
    down_own, down_other = own_first(w_down[0], 1)

    for mask in steps[:-1]:
        rows = jnp.concatenate([rows, swap(rows, mask)], axis=0)
    far = swap(rows, steps[-1])
    in_own, in_other, down_own, down_other = lax.optimization_barrier(
        (in_own, in_other, down_own, down_other)
    )
    n = rows.shape[0] // 2
    one, two = rows[n:], far[:n]
    own = jnp.concatenate(
        [rows[:n], jnp.where(first, one, two), jnp.where(first, two, one), far[n:]], axis=0
    )
    other = swap(own, None)
    h = jnp.dot(own[:, :half], in_own, preferred_element_type=jnp.float32)
    h = h + jnp.dot(other[:, :half], in_other, preferred_element_type=jnp.float32)
    pair = own[:, half:].astype(jnp.float32) + other[:, half:].astype(jnp.float32)
    mine = (jnp.arange(lanes, dtype=jnp.int32) == lax.axis_index("ep"))[None, :]
    score = jnp.sum(jnp.where(mine, pair, 0.0), axis=1, keepdims=True)
    act = clamped_unit(h[:, :hidden], h[:, hidden:]).astype(jnp.bfloat16)

    given = jnp.dot(act, down_other, preferred_element_type=jnp.float32).astype(jnp.bfloat16)
    taken = swap(given, None)
    kept = jnp.dot(act, down_own, preferred_element_type=jnp.float32)
    total = (kept + taken.astype(jnp.float32)) * score
    one, two = total[n : 2 * n], total[2 * n : 3 * n]
    near = jnp.concatenate([total[:n], jnp.where(first, one, two)], axis=0)
    far = jnp.concatenate([jnp.where(first, two, one), total[3 * n :]], axis=0)
    for mask in reversed(steps):
        near = near + swap(far.astype(jnp.bfloat16), mask).astype(jnp.float32)
        n = near.shape[0] // 2
        if mask is not steps[0]:
            near, far = near[:n], near[n:]
    mixed = finish(near)
    theirs = swap(mixed, None)
    return jnp.concatenate(
        [jnp.where(first, mixed, theirs), jnp.where(first, theirs, mixed)], axis=1
    )


def body(tokens, norm_gain, routes, gate_scores, w_gate, w_up, w_down):
    args = (tokens, norm_gain, routes, gate_scores, w_gate, w_up, w_down)
    count = tokens.shape[0]
    top = routes.shape[1]
    nexp = lax.axis_size("ep")
    capacity = max(2, min(count, 2 * count * top // nexp))
    if capacity == count and nexp >= 4 and nexp & (nexp - 1) == 0 and lax.axis_size("tp") == 2:
        return dense(*args)
    return slotted(*args, capacity)


def solution(mesh):
    in_specs = (
        P(("grp", "ep"), None),
        P(),
        P(("grp", "ep"), None),
        P(("grp", "ep"), None),
        P("ep", None, "tp"),
        P("ep", None, "tp"),
        P("ep", "tp", None),
    )
    out_specs = P(("grp", "ep"), None)
    return jax.shard_map(body, mesh=mesh, in_specs=in_specs, out_specs=out_specs, check_vma=False)
```

```python
import jax
import jax.numpy as jnp
from jax import lax
from jax.experimental import pallas as pl
from jax.experimental.pallas import tpu as pltpu
from jax.sharding import PartitionSpec as P


def clamped_unit(g, u):
    gate = jnp.minimum(g, 7.0)
    up = jnp.clip(u, -7.0, 7.0)
    return (up + 1.0) * gate * jax.nn.sigmoid(1.702 * gate)


def expert_rows(rows, wg, wu, wd):
    g = jnp.dot(rows, wg, preferred_element_type=jnp.float32)
    u = jnp.dot(rows, wu, preferred_element_type=jnp.float32)
    act = clamped_unit(g, u).astype(jnp.bfloat16)
    part = jnp.dot(act, wd, preferred_element_type=jnp.float32)
    part = lax.optimization_barrier(part.astype(jnp.bfloat16)).astype(jnp.float32)
    total = lax.psum(part.astype(jnp.bfloat16), "tp")
    return total


def finish(mixed):
    result = mixed.astype(jnp.bfloat16)
    return result


def normalise(tokens, norm_gain):
    xf = tokens.astype(jnp.float32)
    scale = lax.rsqrt(jnp.mean(xf * xf, axis=-1, keepdims=True) + 1e-06)
    return (xf * scale * norm_gain).astype(jnp.bfloat16)


def slot_table(routes, scores, experts, capacity):
    count = routes.shape[0]
    chosen = routes[:, :, None] == experts[None, None, :]
    hit = jnp.any(chosen, axis=1).astype(jnp.int32)
    weight = jnp.sum(jnp.where(chosen, scores[:, :, None], 0.0), axis=1)
    rank = jnp.cumsum(hit, axis=0) - hit
    places = jnp.arange(capacity, dtype=jnp.int32)
    match = (hit[:, :, None] == 1) & (rank[:, :, None] == places[None, None, :])
    row_ids = jnp.arange(count, dtype=jnp.int32)[:, None, None]
    filled = jnp.any(match, axis=0)
    slot_tok = jnp.sum(jnp.where(match, row_ids, 0), axis=0) + count * (
        1 - filled.astype(jnp.int32)
    )
    slot_w = jnp.sum(jnp.where(match, weight[:, :, None], 0.0), axis=0)
    return (slot_tok, slot_w)


def slotted(tokens, norm_gain, routes, gate_scores, w_gate, w_up, w_down, capacity):
    count, width = tokens.shape
    nexp = lax.axis_size("ep")
    wg, wu, wd = (w_gate[0], w_up[0], w_down[0])
    normed = normalise(tokens, norm_gain)
    experts = jnp.arange(nexp, dtype=jnp.int32)
    slot_tok, slot_w = slot_table(routes, gate_scores, experts, capacity)
    padded = jnp.concatenate([normed, jnp.zeros((1, width), jnp.bfloat16)], axis=0)
    outgoing = padded[slot_tok]
    received = lax.all_to_all(outgoing, "ep", split_axis=0, concat_axis=0, tiled=True)
    sources, places, _ = received.shape
    outputs = expert_rows(received.reshape(sources * places, width), wg, wu, wd)
    returned = lax.all_to_all(
        outputs.reshape(sources, places, outputs.shape[1]),
        "ep",
        split_axis=0,
        concat_axis=0,
        tiled=True,
    )
    flat_tok = slot_tok.reshape(-1)
    token_ids = jnp.arange(count, dtype=jnp.int32)
    combine = jnp.where(flat_tok[None, :] == token_ids[:, None], slot_w.reshape(-1)[None, :], 0.0)
    mixed = jnp.dot(
        combine,
        returned.reshape(-1, returned.shape[2]).astype(jnp.float32),
        precision=lax.Precision.HIGHEST,
    )
    return finish(mixed)


def swap(x, mask):
    nexp, cores = lax.axis_size("ep"), lax.axis_size("tp")
    if mask is None:
        return lax.ppermute(x, "tp", [(c, c ^ 1) for c in range(cores)])
    pairs = [(e * cores + c, (e ^ mask[c]) * cores + c) for e in range(nexp) for c in range(cores)]
    return lax.ppermute(x, ("ep", "tp"), pairs)


def prepare(tokens, norm_gain, routes, gate_scores, lanes):
    count, width = tokens.shape
    half = width // 2
    top = routes.shape[1]

    def kernel(*refs):
        given, out_ref, local, sem = refs[:4], refs[4], refs[5:9], refs[9]
        copies = [pltpu.make_async_copy(a, b, sem.at[i]) for i, (a, b) in enumerate(zip(given, local))]
        for copy in copies:
            copy.start()
        for copy in copies:
            copy.wait()
        x_ref, gain_ref, route_ref, score_ref = local
        first = lax.axis_index("tp") == 0
        x = x_ref[...].astype(jnp.float32)
        scale = lax.rsqrt(jnp.mean(x * x, axis=-1, keepdims=True) + 1e-06)
        normed = x * scale * gain_ref[...]
        out_ref[:, :half] = jnp.where(first, normed[:, :half], normed[:, half:]).astype(jnp.bfloat16)
        expert = lax.broadcasted_iota(jnp.int32, (lanes, count), 0)
        weight = jnp.zeros((lanes, count), jnp.float32)
        for k in range(top):
            weight += jnp.where(route_ref[k : k + 1, :] == expert, score_ref[k : k + 1, :], 0.0)
        high = weight.astype(jnp.bfloat16)
        low = (weight - high.astype(jnp.float32)).astype(jnp.bfloat16)
        term = jnp.where(first, high.astype(jnp.float32), low.astype(jnp.float32)).astype(jnp.bfloat16)
        row = lax.broadcasted_iota(jnp.int32, (lanes, lanes), 0)
        col = lax.broadcasted_iota(jnp.int32, (lanes, lanes), 1)
        unit = jnp.where(row == col, 1.0, 0.0).astype(jnp.bfloat16)
        turned = lax.dot_general(term, unit, (((0,), (0,)), ((), ())), preferred_element_type=jnp.float32)
        out_ref[:, half:] = turned.astype(jnp.bfloat16)

    args = (tokens, norm_gain[None, :], routes.T, gate_scores.T)
    return pl.pallas_call(
        kernel,
        in_specs=[pl.BlockSpec(memory_space=pltpu.HBM)] * len(args),
        out_shape=pltpu.VMEM((count, half + lanes), jnp.bfloat16),
        scratch_shapes=[pltpu.VMEM(a.shape, a.dtype) for a in args]
        + [pltpu.SemaphoreType.DMA((len(args),))],
        compiler_params=pltpu.CompilerParams(vmem_limit_bytes=4 << 20),
        name="prepare",
    )(*[pltpu.with_memory_space_constraint(a, pltpu.HBM) for a in args])


def dense(tokens, norm_gain, routes, gate_scores, w_gate, w_up, w_down):
    width = tokens.shape[1]
    nexp = lax.axis_size("ep")
    half = width // 2
    hidden = w_gate.shape[2]
    tp = lax.axis_index("tp")
    first = tp == 0
    masks = [1 << b for b in reversed(range((nexp - 1).bit_length()))]
    steps = list(zip(masks, masks[:-2] + masks[-1:] + masks[-2:-1]))
    lanes = -(-nexp // 128) * 128

    rows = prepare(tokens, norm_gain, routes, gate_scores, lanes)

    def own_first(w, axis):
        own = lax.dynamic_slice_in_dim(w, tp * half, half, axis)
        return own, lax.dynamic_slice_in_dim(w, (1 - tp) * half, half, axis)

    gate_own, gate_other = own_first(w_gate[0], 0)
    up_own, up_other = own_first(w_up[0], 0)
    in_own = jnp.concatenate([gate_own, up_own], axis=1)
    in_other = jnp.concatenate([gate_other, up_other], axis=1)
    down_own, down_other = own_first(w_down[0], 1)

    for mask in steps[:-1]:
        rows = jnp.concatenate([rows, swap(rows, mask)], axis=0)
    far = swap(rows, steps[-1])
    in_own, in_other, down_own, down_other = lax.optimization_barrier(
        (in_own, in_other, down_own, down_other)
    )
    n = rows.shape[0] // 2
    one, two = rows[n:], far[:n]
    own = jnp.concatenate(
        [rows[:n], jnp.where(first, one, two), jnp.where(first, two, one), far[n:]], axis=0
    )
    other = swap(own, None)
    h = jnp.dot(other[:, :half], in_other, preferred_element_type=jnp.float32)
    h = h + jnp.dot(own[:, :half], in_own, preferred_element_type=jnp.float32)
    pair = own[:, half:].astype(jnp.float32) + other[:, half:].astype(jnp.float32)
    mine = (jnp.arange(lanes, dtype=jnp.int32) == lax.axis_index("ep"))[None, :]
    score = jnp.sum(jnp.where(mine, pair, 0.0), axis=1, keepdims=True)
    act = clamped_unit(h[:, :hidden], h[:, hidden:]).astype(jnp.bfloat16)

    given = jnp.dot(act, down_other, preferred_element_type=jnp.float32).astype(jnp.bfloat16)
    taken = swap(given, None)
    kept = jnp.dot(act, down_own, preferred_element_type=jnp.float32)
    total = (kept + taken.astype(jnp.float32)) * score
    one, two = total[n : 2 * n], total[2 * n : 3 * n]
    near = jnp.concatenate([total[:n], jnp.where(first, one, two)], axis=0)
    far = jnp.concatenate([jnp.where(first, two, one), total[3 * n :]], axis=0)
    for mask in reversed(steps):
        near = near + swap(far.astype(jnp.bfloat16), mask).astype(jnp.float32)
        n = near.shape[0] // 2
        if mask is not steps[0]:
            near, far = near[:n], near[n:]
    mixed = finish(near)
    theirs = swap(mixed, None)
    return jnp.concatenate(
        [jnp.where(first, mixed, theirs), jnp.where(first, theirs, mixed)], axis=1
    )


def body(tokens, norm_gain, routes, gate_scores, w_gate, w_up, w_down):
    args = (tokens, norm_gain, routes, gate_scores, w_gate, w_up, w_down)
    count = tokens.shape[0]
    top = routes.shape[1]
    nexp = lax.axis_size("ep")
    capacity = max(2, min(count, 2 * count * top // nexp))
    if capacity == count and nexp >= 4 and nexp & (nexp - 1) == 0 and lax.axis_size("tp") == 2:
        return dense(*args)
    return slotted(*args, capacity)


def solution(mesh):
    in_specs = (
        P(("grp", "ep"), None),
        P(),
        P(("grp", "ep"), None),
        P(("grp", "ep"), None),
        P("ep", None, "tp"),
        P("ep", None, "tp"),
        P("ep", "tp", None),
    )
    out_specs = P(("grp", "ep"), None)
    return jax.shard_map(body, mesh=mesh, in_specs=in_specs, out_specs=out_specs, check_vma=False)
```
